32 devices in a mesh: kv: 4 (over y, x), tp: 8 (over z, core).
Axes of the slice: x: 2, y: 2, z: 4, core: 2. Of those that a mesh axis runs over, the one named last changes fastest.
Arguments:
- tokens: bfloat16 [12, 4096], P(None, ('kv', 'tp')), may hold values from -60 to 60
- gain_pre1: float32 [4096], P('kv'), may hold values from 0.1 to 1.9
- gain_post1: float32 [4096], P('kv'), may hold values from 0.1 to 1.9
- w_gate1: bfloat16 [4096, 11264], P('kv', 'tp'), may hold values from -0.09375 to 0.09375
- w_up1: bfloat16 [4096, 11264], P('kv', 'tp'), may hold values from -0.09375 to 0.09375
- w_down1: bfloat16 [11264, 4096], P('tp', 'kv'), may hold values from -0.078125 to 0.078125
- gain_pre2: float32 [4096], P('kv'), may hold values from 0.1 to 1.9
- gain_post2: float32 [4096], P('kv'), may hold values from 0.1 to 1.9
- w_query: bfloat16 [4096, 4096], P('kv', 'tp'), may hold values from -0.09375 to 0.09375
- w_key: bfloat16 [4096, 2048], P('kv', 'tp'), may hold values from -0.09375 to 0.09375
- w_value: bfloat16 [4096, 2048], P('kv', 'tp'), may hold values from -0.09375 to 0.09375
- w_forget: bfloat16 [4096, 32], replicated, may hold values from -0.09375 to 0.09375
- forget_bias: float32 [32], P('tp'), may hold values from -4 to 4
- w_out: bfloat16 [4096, 4096], P('tp', 'kv'), may hold values from -0.125 to 0.125
- keys_t: bfloat16 [12, 32, 64, 4096], P(None, 'tp', None, 'kv'), may hold values from -250 to 250
- values_t: bfloat16 [12, 32, 64, 4096], P(None, 'tp', None, 'kv'), may hold values from -6 to 6
- decays: float32 [12, 32, 4096], P(None, 'tp', 'kv'), may hold values from -1024 to 0, as said below
- gain_pre3: float32 [4096], P('kv'), may hold values from 0.1 to 1.9
- gain_post3: float32 [4096], P('kv'), may hold values from 0.1 to 1.9
- w_gate2: bfloat16 [4096, 11264], P('kv', 'tp'), may hold values from -0.09375 to 0.09375
- w_up2: bfloat16 [4096, 11264], P('kv', 'tp'), may hold values from -0.09375 to 0.09375
- w_down2: bfloat16 [11264, 4096], P('tp', 'kv'), may hold values from -0.078125 to 0.078125
Outputs:
- mixed_out: bfloat16 [12, 4096], P(None, ('kv', 'tp'))
The draws below stay inside these ranges and needn't reach their ends.
Inputs may be any that keep to these rules, and one draw needn't show every extreme that they name: `decays`: each sequence's and head's values do not fall along the positions and end at 0 at the last position.
All inputs are finite; a program needn't handle non-finite values.
Results may differ from the reference program's by a relative error of at most 0.012.
Values may be sent and summed in bfloat16 or wider, within the bound.
A program may use at most 64 MiB of HBM per device.

```python
import jax
import jax.numpy as jnp
from jax import lax

D = 4096
HEADS = 64
KEY_VALUE_HEADS = 32
HEAD = 64
FF = 11264
SEQUENCE_COUNT = 12
POS_DEV = 1024
CONTEXT_LENGTH = 4096
N_KV = 4
N_TP = 8


def draw_tokens(key, part):
    random_subkeys = jax.random.split(key, 3)
    column = jnp.arange(D)
    along_kv = column // (D // N_KV) / max(N_KV - 1, 1)
    along_tp = column // (D // (N_KV * N_TP)) % N_TP / max(N_TP - 1, 1)
    jitter = jax.random.uniform(random_subkeys[0], (D,), jnp.float32, 0.5, 1.5)
    col_scale = 3.0 ** along_kv * 3.0 ** along_tp * jitter / 4.0
    row_scale = 10.0 ** jax.random.uniform(random_subkeys[1], (SEQUENCE_COUNT, 1), jnp.float32, -0.5, 0.5)
    sample = jax.random.normal(random_subkeys[2], (SEQUENCE_COUNT, D), jnp.float32)
    sample = jnp.clip(sample, -5.0, 5.0)
    return (sample * col_scale[None, :] * row_scale).astype(jnp.bfloat16)


def draw_keys_t(key, part):
    random_subkeys = jax.random.split(key, 1)
    full_shape = (SEQUENCE_COUNT, KEY_VALUE_HEADS, HEAD, CONTEXT_LENGTH)
    sample = jax.random.normal(random_subkeys[0], full_shape, jnp.float32)
    return sample.astype(jnp.bfloat16)


def draw_decays(key, part):
    random_subkeys = jax.random.split(key, 7)
    slow_share = 0.5
    sluggish_head = jax.random.uniform(random_subkeys[0], (1, KEY_VALUE_HEADS, 1), jnp.float32) < slow_share
    blocks = CONTEXT_LENGTH // POS_DEV
    block_factor = 2.0 ** jax.random.uniform(random_subkeys[1], (SEQUENCE_COUNT, KEY_VALUE_HEADS, blocks), jnp.float32, -1.0, 1.0)
    block_factor = jnp.repeat(block_factor, POS_DEV, axis=2)
    jitter = jax.random.uniform(random_subkeys[2], (SEQUENCE_COUNT, KEY_VALUE_HEADS, CONTEXT_LENGTH), jnp.float32, 0.3, 1.7)
    slow_rate = jax.random.uniform(random_subkeys[3], (SEQUENCE_COUNT, KEY_VALUE_HEADS, 1), jnp.float32, 0.2, 0.6) / CONTEXT_LENGTH
    fast_rate = 1.0 / jax.random.uniform(random_subkeys[4], (SEQUENCE_COUNT, KEY_VALUE_HEADS, 1), jnp.float32, 15.0, 40.0)
    logarithm_rate = jnp.where(sluggish_head, slow_rate, fast_rate) * jitter * block_factor
    spike_position = jax.random.randint(random_subkeys[5], (SEQUENCE_COUNT, KEY_VALUE_HEADS, 2), 0, CONTEXT_LENGTH)
    forgotten_fraction = -jnp.log(jax.random.uniform(random_subkeys[6], (SEQUENCE_COUNT, KEY_VALUE_HEADS, 2), jnp.float32, 0.5, 0.8))
    token_position = jnp.arange(CONTEXT_LENGTH)
    spike_tokens = jnp.sum((token_position[None, None, None, :] == spike_position[..., None]) * forgotten_fraction[..., None], axis=2)
    logarithm_rate = logarithm_rate + jnp.where(sluggish_head, spike_tokens, 0.0)
    remaining = jnp.cumsum(logarithm_rate[..., ::-1], axis=-1)[..., ::-1] - logarithm_rate
    return -remaining


def raised(values, own_key, source, target, parts, factor):
    owner, partner = [(jnp.arange(values.shape[axis_at]) // (values.shape[axis_at] // parts)).reshape([-1 if axis == axis_at else 1 for axis in range(values.ndim)]) for axis_at in (source, target)]
    chosen = jax.random.permutation(own_key, parts)[partner]
    strong = (owner == chosen) | (owner == (partner + parts // 2) % parts)
    return jnp.where(strong, factor * values, values)


def block_levels(own_key, dims, shards, low, high):
    level = 1.0
    for axis_at, parts in shards:
        steps = jax.random.uniform(jax.random.fold_in(jax.random.fold_in(own_key, 6), axis_at), (parts,), jnp.float32, low / len(shards), high / len(shards))
        level = level * jnp.repeat(jnp.exp(steps), dims[axis_at] // parts).reshape((-1,) + (1,) * (len(dims) - 1 - axis_at))
    return level


def gaussian(own_key, extent, width, limit, cuts=(), dtype=jnp.bfloat16):
    values = jax.random.normal(own_key, extent, jnp.float32) * width
    if len(cuts) > 0:
        values = block_levels(own_key, extent, cuts, -0.22, 0.18) * values
    return jnp.clip(values, min=-limit, max=limit).astype(dtype)


def bell_draw_with(key, dims, width, limit, cuts, heavy, kind=jnp.bfloat16):
    values = width * jax.random.normal(key, dims, jnp.float32)
    if cuts:
        values = values * block_levels(key, dims, cuts, -0.22, 0.18)
    return jnp.clip(raised(values, jax.random.fold_in(key, 3), *heavy), -limit, limit).astype(kind)


def setup_inputs(seed: int = 0) -> dict:
    keys = jax.random.split(jax.random.key(seed), 23)
    tokens = draw_tokens(jax.random.fold_in(keys[22], 71), 0)
    gain_pre1 = jnp.clip(1.0 + 0.18 * jax.random.normal(keys[1], (D,), jnp.float32), 0.1, 1.9)
    gain_post1 = jnp.clip(1.0 + 0.18 * jax.random.normal(keys[2], (D,), jnp.float32), 0.1, 1.9)
    w_gate1 = gaussian(keys[3], (D, FF), D ** -0.5, 0.09375, ((0, 4), (1, 8)))
    w_up1 = gaussian(keys[4], (D, FF), D ** -0.5, 0.09375, ((0, 4), (1, 8)))
    w_down1 = bell_draw_with(keys[5], (FF, D), FF ** -0.5, 0.078125, ((0, 8), (1, 4)), (0, 1, 8, 2.0))
    gain_pre2 = jnp.clip(1.0 + 0.18 * jax.random.normal(keys[6], (D,), jnp.float32), 0.1, 1.9)
    gain_post2 = jnp.clip(1.0 + 0.18 * jax.random.normal(keys[7], (D,), jnp.float32), 0.1, 1.9)
    w_query = gaussian(keys[8], (D, HEADS * HEAD), D ** -0.5, 0.09375, ((0, 4), (1, 8)))
    w_key = gaussian(keys[9], (D, KEY_VALUE_HEADS * HEAD), D ** -0.5, 0.09375, ((0, 4), (1, 8)))
    w_value = gaussian(keys[10], (D, KEY_VALUE_HEADS * HEAD), D ** -0.5, 0.09375, ((0, 4), (1, 8)))
    w_forget = gaussian(keys[11], (D, KEY_VALUE_HEADS), D ** -0.5, 0.09375)
    forget_bias = gaussian(keys[12], (KEY_VALUE_HEADS,), 1.0, 4.0, ((0, 8),), jnp.float32)
    w_out = bell_draw_with(keys[13], (HEADS * HEAD, D), (HEADS * HEAD) ** -0.5, 0.125, ((0, 8), (1, 4)), (0, 1, 8, 2.0))
    keys_t = draw_keys_t(jax.random.fold_in(keys[22], 71), 0)
    values_t = gaussian(keys[15], (SEQUENCE_COUNT, KEY_VALUE_HEADS, HEAD, CONTEXT_LENGTH), 1.0, 6.0, ((1, 8), (3, 4)))
    decays = draw_decays(jax.random.fold_in(keys[22], 71), 0)
    gain_pre3 = jnp.clip(1.0 + 0.18 * jax.random.normal(keys[17], (D,), jnp.float32), 0.1, 1.9)
    gain_post3 = jnp.clip(1.0 + 0.18 * jax.random.normal(keys[18], (D,), jnp.float32), 0.1, 1.9)
    w_gate2 = gaussian(keys[19], (D, FF), D ** -0.5, 0.09375, ((0, 4), (1, 8)))
    w_up2 = gaussian(keys[20], (D, FF), D ** -0.5, 0.09375, ((0, 4), (1, 8)))
    w_down2 = bell_draw_with(keys[21], (FF, D), FF ** -0.5, 0.078125, ((0, 8), (1, 4)), (0, 1, 8, 2.0))
    return dict(tokens=tokens, gain_pre1=gain_pre1, gain_post1=gain_post1, w_gate1=w_gate1, w_up1=w_up1, w_down1=w_down1, gain_pre2=gain_pre2, gain_post2=gain_post2, w_query=w_query, w_key=w_key, w_value=w_value, w_forget=w_forget, forget_bias=forget_bias, w_out=w_out, keys_t=keys_t, values_t=values_t, decays=decays, gain_pre3=gain_pre3, gain_post3=gain_post3, w_gate2=w_gate2, w_up2=w_up2, w_down2=w_down2)


EPSILON = 1e-06

def pre_norm(hidden_rows, gain):
    widened = hidden_rows.astype(jnp.float32)
    inv_rms = lax.rsqrt(lax.optimization_barrier(jnp.mean(widened * widened, axis=1, keepdims=True)) + EPSILON)
    scaled = (widened * gain[None, :]).astype(jnp.bfloat16)
    return (scaled, inv_rms)

def post_add(hidden_rows, branch, gain, factor):
    inv_rms = lax.rsqrt(lax.optimization_barrier(jnp.mean(branch * branch, axis=1, keepdims=True)) + EPSILON)
    return (hidden_rows.astype(jnp.float32) + factor * branch * inv_rms * gain[None, :]).astype(jnp.bfloat16)

def channel_mix(hidden_rows, gain_pre, gain_post, w_gate, w_up, w_down, factor):
    scaled, inv_rms = pre_norm(hidden_rows, gain_pre)
    gate = jnp.dot(scaled, w_gate, preferred_element_type=jnp.float32) * inv_rms
    upward = jnp.dot(scaled, w_up, preferred_element_type=jnp.float32) * inv_rms
    hidden = (jax.nn.silu(gate) * upward).astype(jnp.bfloat16)
    branch = jnp.dot(hidden, w_down, preferred_element_type=jnp.float32)
    return post_add(hidden_rows, branch, gain_post, factor)

def token_mix(hidden_rows, gain_pre, gain_post, w_query, w_key, w_value, w_forget, forget_bias, w_out, keys_t, values_t, decays):
    scaled, inv_rms = pre_norm(hidden_rows, gain_pre)
    group_size = HEADS // KEY_VALUE_HEADS
    query_rows = (jnp.dot(scaled, w_query, preferred_element_type=jnp.float32) * inv_rms).astype(jnp.bfloat16)
    query_rows = query_rows.reshape(SEQUENCE_COUNT, KEY_VALUE_HEADS, group_size, HEAD)
    fresh_key = (jnp.dot(scaled, w_key, preferred_element_type=jnp.float32) * inv_rms).astype(jnp.bfloat16)
    fresh_key = fresh_key.reshape(SEQUENCE_COUNT, KEY_VALUE_HEADS, HEAD)
    value_new = (jnp.dot(scaled, w_value, preferred_element_type=jnp.float32) * inv_rms).astype(jnp.bfloat16)
    value_new = value_new.reshape(SEQUENCE_COUNT, KEY_VALUE_HEADS, HEAD)
    log_gate = jax.nn.log_sigmoid(jnp.dot(scaled, w_forget, preferred_element_type=jnp.float32) * inv_rms + forget_bias[None, :])

    def attend(operands):
        query_one, keys_one, values_one, decay_one, gate_one, key_one, value_one = operands
        query_wide = query_one.astype(jnp.float32)
        scores = jnp.einsum('kgd,kdp->kgp', query_wide, keys_one.astype(jnp.float32)) * HEAD ** (-0.5)
        scores = scores + decay_one[:, None, :] + gate_one[:, None, None]
        blocked = scores.reshape(KEY_VALUE_HEADS, group_size, N_KV, POS_DEV)
        block_max = lax.optimization_barrier(jnp.max(blocked, axis=3))
        weights = jnp.exp(blocked - block_max[..., None])
        block_sum = lax.optimization_barrier(jnp.sum(weights, axis=3))
        rounded = lax.optimization_barrier(weights.astype(jnp.bfloat16)).astype(jnp.float32)
        values_blocked = values_one.reshape(KEY_VALUE_HEADS, HEAD, N_KV, POS_DEV).astype(jnp.float32)
        block_values = jnp.einsum('kgnp,kdnp->kgnd', rounded, values_blocked)
        own_score = jnp.einsum('kgd,kd->kg', query_wide, key_one.astype(jnp.float32)) * HEAD ** (-0.5)
        peak_all = jnp.maximum(lax.optimization_barrier(jnp.max(block_max, axis=2)), own_score)
        block_scale = jnp.exp(block_max - peak_all[..., None])
        own_weight = jnp.exp(own_score - peak_all)
        denominator = lax.optimization_barrier(jnp.sum(block_sum * block_scale, axis=2)) + own_weight
        numerator = lax.optimization_barrier(jnp.sum(block_values * block_scale[..., None], axis=2))
        numerator = numerator + own_weight[..., None] * value_one.astype(jnp.float32)[:, None, :]
        return (numerator / denominator[..., None]).astype(jnp.bfloat16)
    attended = lax.map(attend, (query_rows, keys_t, values_t, decays, log_gate, fresh_key, value_new))
    attended = attended.reshape(SEQUENCE_COUNT, HEADS * HEAD)
    branch = jnp.dot(attended, w_out, preferred_element_type=jnp.float32)
    return post_add(hidden_rows, branch, gain_post, 1.0)

def reference(tokens, gain_pre1, gain_post1, w_gate1, w_up1, w_down1, gain_pre2, gain_post2, w_query, w_key, w_value, w_forget, forget_bias, w_out, keys_t, values_t, decays, gain_pre3, gain_post3, w_gate2, w_up2, w_down2):
    first = channel_mix(tokens, gain_pre1, gain_post1, w_gate1, w_up1, w_down1, 0.5)
    second = token_mix(first, gain_pre2, gain_post2, w_query, w_key, w_value, w_forget, forget_bias, w_out, keys_t, values_t, decays)
    return channel_mix(second, gain_pre3, gain_post3, w_gate2, w_up2, w_down2, 0.5)
```

```python
import functools

import jax
import jax.numpy as jnp
from jax import lax
from jax.experimental import pallas as pl
from jax.experimental.pallas import tpu as pltpu
from jax.sharding import PartitionSpec as P

D = 4096
HEAD = 64


EPSILON = 1e-06


def joined(x, axis, combine):
    everything = jax.tree.map(lambda part: lax.all_gather(part, axis), x)
    initial = jax.tree.map(lambda part: part[0], everything)

    def lap(k, so_far):
        return combine(so_far, jax.tree.map(lambda part: part[k], everything))

    return lax.fori_loop(1, lax.axis_size(axis), lap, initial)


def add_branch(row_block, mixed, weight_out, gain_post, factor):
    branch = lax.psum(jnp.dot(mixed, weight_out, preferred_element_type=jnp.float32), "tp")
    summed = lax.psum(jnp.sum(branch * branch, axis=1), "kv")
    inv_rms = lax.rsqrt(summed / D + EPSILON)[:, None]
    return (row_block.astype(jnp.float32) + factor * branch * inv_rms * gain_post[None, :]).astype(
        jnp.bfloat16
    )


def channel_mix(row_block, gain_pre, gain_post, w_gate, w_up, w_down, factor):
    widened = row_block.astype(jnp.float32)
    scaled = (widened * gain_pre[None, :]).astype(jnp.bfloat16)
    square = jnp.sum(widened * widened, axis=1)
    gate_part = jnp.dot(scaled, w_gate, preferred_element_type=jnp.float32)
    up_part = jnp.dot(scaled, w_up, preferred_element_type=jnp.float32)
    gate, upward, summed = lax.psum((gate_part, up_part, square), "kv")
    inv_rms = lax.rsqrt(summed / D + EPSILON)[:, None]
    hidden = (jax.nn.silu(gate * inv_rms) * (upward * inv_rms)).astype(jnp.bfloat16)
    return add_branch(row_block, hidden, w_down, gain_post, factor)


def merge_softmax(former, latter):
    joined_max = jnp.maximum(former[0], latter[0])
    former_scale = jnp.exp(former[0] - joined_max)
    latter_scale = jnp.exp(latter[0] - joined_max)
    return (
        joined_max,
        former[1] * former_scale + latter[1] * latter_scale,
        former[2] * former_scale[..., None] + latter[2] * latter_scale[..., None],
    )


def token_mix(
    row_block,
    gain_pre,
    gain_post,
    w_query,
    w_key,
    w_value,
    w_forget,
    forget_bias,
    w_out,
    keys_t,
    values_t,
    decays,
):
    widened = row_block.astype(jnp.float32)
    scaled = (widened * gain_pre[None, :]).astype(jnp.bfloat16)
    square = jnp.sum(widened * widened, axis=1)
    rows_dev = row_block.shape[1]
    seq_count = row_block.shape[0]
    kv_dev = w_key.shape[1] // HEAD
    group_size = w_query.shape[1] // w_key.shape[1]
    forget_cols = lax.dynamic_slice(
        w_forget,
        (lax.axis_index("kv") * rows_dev, lax.axis_index("tp") * kv_dev),
        (rows_dev, kv_dev),
    )
    query_part = jnp.dot(scaled, w_query, preferred_element_type=jnp.float32)
    key_part = jnp.dot(scaled, w_key, preferred_element_type=jnp.float32)
    value_part = jnp.dot(scaled, w_value, preferred_element_type=jnp.float32)
    forget_part = jnp.dot(scaled, forget_cols, preferred_element_type=jnp.float32)
    query_rows, fresh_key, value_new, forget, summed = lax.psum(
        (query_part, key_part, value_part, forget_part, square), "kv"
    )
    inv_rms = lax.rsqrt(summed / D + EPSILON)[:, None]
    query_rows = (
        (query_rows * inv_rms).astype(jnp.bfloat16).reshape(seq_count, kv_dev, group_size, HEAD)
    )
    fresh_key = (fresh_key * inv_rms).astype(jnp.bfloat16).reshape(seq_count, kv_dev, HEAD)
    value_new = (value_new * inv_rms).astype(jnp.bfloat16).reshape(seq_count, kv_dev, HEAD)
    log_gate = jax.nn.log_sigmoid(forget * inv_rms + forget_bias[None, :])
    scores = jnp.einsum(
        "bkgd,bkdp->bkgp", query_rows, keys_t, preferred_element_type=jnp.float32
    ) * HEAD ** (-0.5)
    scores = scores + decays[:, :, None, :] + log_gate[:, :, None, None]
    block_max = jnp.max(scores, axis=3)
    weights = jnp.exp(scores - block_max[..., None])
    block_sum = jnp.sum(weights, axis=3)
    block_values = jnp.einsum(
        "bkgp,bkdp->bkgd",
        weights.astype(jnp.bfloat16),
        values_t,
        preferred_element_type=jnp.float32,
    )
    block_max, block_sum, block_values = joined(
        (block_max, block_sum, block_values), "kv", merge_softmax
    )
    own_score = jnp.einsum(
        "tlvi,tli->tlv", query_rows, fresh_key, preferred_element_type=jnp.float32
    ) * HEAD ** (-0.5)
    peak_all = jnp.maximum(block_max, own_score)
    block_scale = jnp.exp(block_max - peak_all)
    own_weight = jnp.exp(own_score - peak_all)
    denominator = block_sum * block_scale + own_weight
    numerator = block_values * block_scale[..., None]
    numerator = numerator + own_weight[..., None] * value_new.astype(jnp.float32)[:, :, None, :]
    attended = (numerator / denominator[..., None]).astype(jnp.bfloat16)
    attended = attended.reshape(seq_count, kv_dev * group_size * HEAD)
    return add_branch(row_block, attended, w_out, gain_post, 1.0)


def body(
    tokens,
    gain_pre1,
    gain_post1,
    w_gate1,
    w_up1,
    w_down1,
    gain_pre2,
    gain_post2,
    w_query,
    w_key,
    w_value,
    w_forget,
    forget_bias,
    w_out,
    keys_t,
    values_t,
    decays,
    gain_pre3,
    gain_post3,
    w_gate2,
    w_up2,
    w_down2,
):
    row_block = lax.all_gather(tokens, "tp", axis=1, tiled=True)
    stream = channel_mix(row_block, gain_pre1, gain_post1, w_gate1, w_up1, w_down1, 0.5)
    stream = token_mix(
        stream,
        gain_pre2,
        gain_post2,
        w_query,
        w_key,
        w_value,
        w_forget,
        forget_bias,
        w_out,
        keys_t,
        values_t,
        decays,
    )
    stream = channel_mix(stream, gain_pre3, gain_post3, w_gate2, w_up2, w_down2, 0.5)
    own_cols = stream.shape[1] // lax.axis_size("tp")
    result = lax.dynamic_slice_in_dim(stream, lax.axis_index("tp") * own_cols, own_cols, 1)
    return result


LANES = 128
F32 = jnp.float32
BF16 = jnp.bfloat16


def fits(mesh, shapes):
    return (
        shapes["cols"] == LANES
        and shapes["hidden"] % LANES == 0
        and shapes["kv_cols"] % LANES == 0
        and shapes["kv_dev"] <= 8
        and shapes["rows_dev"] % (2 * LANES) == 0
        and shapes["query_cols"] == 2 * shapes["kv_cols"]
    )


def layer_kernel(
    n_kv,
    n_tp,
    tokens_ref,
    pre1_ref,
    post1_ref,
    pre2_ref,
    post2_ref,
    pre3_ref,
    post3_ref,
    bias_ref,
    decays_ref,
    gate1_hbm,
    up1_hbm,
    down1_hbm,
    query_hbm,
    key_hbm,
    value_hbm,
    forget_hbm,
    out_hbm,
    keys_hbm,
    values_hbm,
    gate2_hbm,
    up2_hbm,
    down2_hbm,
    result_ref,
    gate1,
    up1,
    down1,
    wq,
    wk,
    wv,
    wf,
    wo,
    keys,
    values,
    gate2,
    up2,
    down2,
    load_sems,
    token_buf,
    stream,
    own_gu,
    gu_a,
    gu_b,
    aux_a,
    aux_b,
    aux_c,
    stat_a,
    stat_b,
    stat_c,
    stat_d,
    qkv_buf,
    grouped_q,
    fresh,
    own_buf,
    soft_buf,
    per_seq,
    branch_buf,
    rs_a,
    rs_b,
    rs_c,
    ag_a,
    ag_b,
    kv_send,
    kv_recv,
    tp_send,
    tp_recv,
):
    kv = lax.axis_index("kv")
    tp = lax.axis_index("tp")
    seqs = tokens_ref.shape[0]
    rows_dev = n_tp * LANES
    kv_cols = wk.shape[1]
    kv_dev = kv_cols // HEAD
    blocks = gate1.shape[1] // LANES

    pairs = (
        (gate1_hbm, gate1),
        (up1_hbm, up1),
        (down1_hbm, down1),
        (query_hbm, wq),
        (key_hbm, wk),
        (value_hbm, wv),
        (forget_hbm.at[pl.ds(pl.multiple_of(kv * rows_dev, rows_dev), rows_dev), :], wf),
        (keys_hbm, keys),
        (values_hbm, values),
        (out_hbm, wo),
        (gate2_hbm, gate2),
        (up2_hbm, up2),
        (down2_hbm, down2),
    )
    loads = [
        pltpu.make_async_copy(source, target, load_sems.at[i])
        for i, (source, target) in enumerate(pairs)
    ]
    for load in loads:
        load.start()

    barrier = pltpu.get_barrier_semaphore()
    for off in range(1, n_kv):
        pl.semaphore_signal(
            barrier,
            inc=1,
            device_id={"kv": lax.rem(kv + off, n_kv)},
            device_id_type=pl.DeviceIdType.MESH,
        )
    for off in range(1, n_tp):
        pl.semaphore_signal(
            barrier,
            inc=1,
            device_id={"tp": lax.rem(tp + off, n_tp)},
            device_id_type=pl.DeviceIdType.MESH,
        )
    pl.semaphore_wait(barrier, n_kv + n_tp - 2)

    sends = []

    def exchange(axis, number, buf, source=None):
        me, n, ssem, rsem = (
            (kv, n_kv, kv_send, kv_recv) if axis == "kv" else (tp, n_tp, tp_send, tp_recv)
        )
        copies = []
        for off in range(1, n):
            peer = lax.rem(me + off, n)
            copy = pltpu.make_async_remote_copy(
                src_ref=buf.at[0] if source is None else source(peer),
                dst_ref=buf.at[off],
                send_sem=ssem.at[number, off - 1],
                recv_sem=rsem.at[number, off - 1],
                device_id={axis: peer},
                device_id_type=pl.DeviceIdType.MESH,
            )
            copy.start()
            copies.append(copy)
        sends.extend(copies)
        return copies

    def arrived(copies):
        for copy in copies:
            copy.wait_recv()

    def slots(buf):
        total = buf[0].astype(F32)
        for off in range(1, buf.shape[0]):
            total += buf[off].astype(F32)
        return total

    def slot_of(place):
        return lax.rem(tp - place + n_tp, n_tp)

    def scaled_stream(gain_ref):
        scaled = [
            (stream[j] * gain_ref[j : j + 1, :]).astype(BF16) for j in range(n_tp)
        ]
        square = stream[0] * stream[0]
        for j in range(1, n_tp):
            square += stream[j] * stream[j]
        return jnp.concatenate(scaled, axis=1), jnp.sum(square, axis=1, keepdims=True)

    def factor_of(total_square):
        return lax.rsqrt(total_square * (1.0 / (n_kv * rows_dev)) + EPSILON)

    def hidden_units(gain_ref, gate_w, up_w, waits, gu_buf, aux_buf, gu_number, aux_number):
        scaled, square = scaled_stream(gain_ref)
        aux_buf[0] = jnp.broadcast_to(square, (seqs, LANES))
        aux_copies = exchange("kv", aux_number, aux_buf)
        for load in waits:
            load.wait()

        def tile(j, carry):
            cols = pl.ds(pl.multiple_of(j * LANES, LANES), LANES)
            both = jnp.concatenate([gate_w[:, cols], up_w[:, cols]], axis=1)
            part = jnp.dot(scaled, both, preferred_element_type=F32)
            own_gu[j] = part
            gu_buf[0, j] = part.astype(BF16)
            return carry

        lax.fori_loop(0, blocks, tile, 0)
        copies = exchange("kv", gu_number, gu_buf)
        arrived(aux_copies)
        inv = factor_of(slots(aux_buf))
        arrived(copies)
        hidden = []
        for j in range(blocks):
            total = own_gu[j]
            for off in range(1, n_kv):
                total += gu_buf[off, j].astype(F32)
            gate = total[:, :LANES] * inv
            upward = total[:, LANES:] * inv
            hidden.append((gate / (1.0 + jnp.exp(-gate)) * upward).astype(BF16))
        return jnp.concatenate(hidden, axis=1)

    def branch_sum(mixed, weight, rs_buf, number):
        def tile(j, carry):
            cols = pl.ds(pl.multiple_of(j * 2 * LANES, 2 * LANES), 2 * LANES)
            part = jnp.dot(mixed, weight[:, cols], preferred_element_type=F32)
            branch_buf[number, 2 * j] = part[:, :LANES]
            branch_buf[number, 2 * j + 1] = part[:, LANES:]
            return carry

        lax.fori_loop(0, n_tp // 2, tile, 0)
        copies = exchange("tp", number, rs_buf, lambda peer: branch_buf.at[number, peer])
        total = branch_buf[number, tp]
        arrived(copies)
        for off in range(1, n_tp):
            total += rs_buf[off]
        return total

    def add_branch_all(own_cols, gain_ref, factor, ag_buf, ag_number, stat_buf, stat_number):
        ag_buf[0] = own_cols
        arrived(exchange("tp", ag_number, ag_buf))
        square = ag_buf[0] * ag_buf[0]
        for off in range(1, n_tp):
            square += ag_buf[off] * ag_buf[off]
        stat_buf[0] = jnp.broadcast_to(jnp.sum(square, axis=1, keepdims=True), (seqs, LANES))
        arrived(exchange("kv", stat_number, stat_buf))
        inv = factor_of(slots(stat_buf)) * factor
        for j in range(n_tp):
            branch = ag_buf[slot_of(j)]
            stream[j] = (
                (stream[j] + branch * inv * gain_ref[j : j + 1, :]).astype(BF16).astype(F32)
            )

    arrived(exchange("tp", 0, token_buf, lambda peer: tokens_ref))
    token_buf[0] = tokens_ref[...]
    for j in range(n_tp):
        stream[j] = token_buf[slot_of(j)].astype(F32)
    hidden = hidden_units(pre1_ref, gate1, up1, loads[0:2], gu_a, aux_a, 0, 1)
    loads[2].wait()
    own_cols = branch_sum(hidden, down1, rs_a, 1)
    add_branch_all(own_cols, post1_ref, 0.5, ag_a, 2, stat_a, 2)

    scaled, square = scaled_stream(pre2_ref)
    for load in loads[3:7]:
        load.wait()
    forget = jnp.dot(scaled, wf[...], preferred_element_type=F32)
    lane = lax.broadcasted_iota(jnp.int32, (seqs, LANES), 1)
    column = lax.broadcasted_iota(jnp.int32, forget.shape, 1)
    aux = jnp.broadcast_to(square, (seqs, LANES))
    for k in range(kv_dev):
        picked = jnp.sum(
            jnp.where(column == tp * kv_dev + k, forget, 0.0), axis=1, keepdims=True
        )
        aux = jnp.where(lane == k, picked, aux)
    aux_b[0] = aux
    aux_copies = exchange("kv", 3, aux_b)
    query_cols = wq.shape[1]
    step = 2 * LANES
    for j in range(query_cols // step):
        qkv_buf[0, :, j * step : (j + 1) * step] = jnp.dot(
            scaled, wq[:, j * step : (j + 1) * step], preferred_element_type=F32
        )
    qkv_buf[0, :, query_cols : query_cols + kv_cols] = jnp.dot(
        scaled, wk[...], preferred_element_type=F32
    )
    qkv_buf[0, :, query_cols + kv_cols :] = jnp.dot(scaled, wv[...], preferred_element_type=F32)
    qkv_copies = exchange("kv", 4, qkv_buf)

    row_at = lax.broadcasted_iota(jnp.int32, (query_cols, kv_cols), 0)
    col_at = lax.broadcasted_iota(jnp.int32, (query_cols, kv_cols), 1)
    selects = [
        jnp.where(
            row_at == (lax.div(col_at, HEAD) * 2 + g) * HEAD + lax.rem(col_at, HEAD), 1.0, 0.0
        ).astype(BF16)
        for g in range(2)
    ]
    arrived(aux_copies)
    aux = slots(aux_b)
    inv = factor_of(aux[:, kv_dev : kv_dev + 1])
    bias = jnp.zeros((seqs, LANES), F32)
    for k in range(kv_dev):
        bias = jnp.where(lane == k, bias_ref[k], bias)
    logit = aux * inv + bias
    log_gate = jnp.minimum(logit, 0.0) - jnp.log(1.0 + jnp.exp(-jnp.abs(logit)))
    log_gate = jnp.where(lane < kv_dev, log_gate, 0.0)
    arrived(qkv_copies)
    qkv = (slots(qkv_buf) * inv).astype(BF16)
    queries = qkv[:, :query_cols]
    for g in range(2):
        grouped_q[g] = jnp.dot(queries, selects[g], preferred_element_type=F32)
    fresh[0] = qkv[:, query_cols : query_cols + kv_cols].astype(F32)
    fresh[1] = qkv[:, query_cols + kv_cols :].astype(F32)
    loads[7].wait()
    loads[8].wait()

    heads = 2 * kv_dev
    head_row = lax.broadcasted_iota(jnp.int32, (heads, kv_cols), 0)
    head_col = lax.div(lax.broadcasted_iota(jnp.int32, (heads, kv_cols), 1), HEAD)
    diagonal = lax.rem(head_row, kv_dev) == head_col
    first_group = head_row < kv_dev
    stat_row = lax.broadcasted_iota(jnp.int32, (heads, LANES), 0)
    stat_lane = lax.broadcasted_iota(jnp.int32, (heads, LANES), 1)
    stat_diag = lax.rem(stat_row, kv_dev) == stat_lane

    def folded(x, g):
        return jnp.sum(x[g * kv_dev : (g + 1) * kv_dev], axis=0, keepdims=True)

    def sequence(b):
        q0 = grouped_q[0, pl.ds(b, 1), :]
        q1 = grouped_q[1, pl.ds(b, 1), :]
        spread = jnp.where(diagonal, jnp.where(first_group, q0, q1), 0.0)
        scores = jnp.dot(spread.astype(BF16), keys[b], preferred_element_type=F32)
        decay = decays_ref[b]
        scores = scores * HEAD ** (-0.5) + jnp.concatenate([decay, decay], axis=0)
        block_max = jnp.max(scores, axis=1, keepdims=True)
        weights = jnp.exp(scores - block_max)
        block_sum = jnp.sum(weights, axis=1, keepdims=True)
        block_values = lax.dot_general(
            weights.astype(BF16), values[b], (((1,), (1,)), ((), ())), preferred_element_type=F32
        )
        block_values = jnp.where(diagonal, block_values, 0.0)
        own = jnp.sum(spread * fresh[0, pl.ds(b, 1), :], axis=1, keepdims=True) * HEAD ** (-0.5)
        max_at = jnp.where(stat_diag, block_max, 0.0)
        sum_at = jnp.where(stat_diag, block_sum, 0.0)
        own_at = jnp.where(stat_diag, own, 0.0)
        found = jnp.concatenate([block_values, max_at, sum_at, own_at], axis=1)
        per_seq[b] = jnp.concatenate([folded(found, 0), folded(found, 1)], axis=0)

    def sequences(i, carry):
        for u in range(UNROLL):
            sequence(i * UNROLL + u)
        return carry

    lax.fori_loop(0, seqs // UNROLL, sequences, 0)
    width = kv_cols + 2 * LANES
    for g in range(2):
        for b in range(seqs):
            soft_buf[0, g, b : b + 1, :] = per_seq[b, g : g + 1, :width]
            own_buf[g, b : b + 1, :] = per_seq[b, g : g + 1, width:]
    soft_copies = exchange("kv", 5, soft_buf)
    arrived(soft_copies)

    wide_col = lax.div(lax.broadcasted_iota(jnp.int32, (seqs, kv_cols), 1), HEAD)

    def widened(x):
        wide = jnp.broadcast_to(x[:, 0:1], (seqs, kv_cols))
        for k in range(1, kv_dev):
            wide = jnp.where(wide_col == k, x[:, k : k + 1], wide)
        return wide

    attended = None
    for g in range(2):
        maxima = [
            soft_buf[off, g, :, kv_cols : kv_cols + LANES] + log_gate for off in range(n_kv)
        ]
        peak = own_buf[g]
        for maximum in maxima:
            peak = jnp.maximum(peak, maximum)
        own_weight = jnp.exp(own_buf[g] - peak)
        denominator = own_weight
        numerator = widened(own_weight) * fresh[1]
        for off in range(n_kv):
            scale = jnp.exp(maxima[off] - peak)
            denominator += scale * soft_buf[off, g, :, kv_cols + LANES :]
            numerator += widened(scale) * soft_buf[off, g, :, :kv_cols]
        part = (numerator / widened(denominator)).astype(BF16)
        moved = lax.dot_general(
            part, selects[g], (((1,), (1,)), ((), ())), preferred_element_type=F32
        )
        attended = moved if attended is None else attended + moved
    loads[9].wait()
    own_cols = branch_sum(attended.astype(BF16), wo, rs_b, 3)
    add_branch_all(own_cols, post2_ref, 1.0, ag_b, 4, stat_b, 6)

    hidden = hidden_units(pre3_ref, gate2, up2, loads[10:12], gu_b, aux_c, 7, 8)
    loads[12].wait()
    own_cols = branch_sum(hidden, down2, rs_c, 5)
    square = jnp.sum(own_cols * own_cols, axis=1, keepdims=True)
    stat_c[0] = jnp.broadcast_to(square, (seqs, LANES))
    arrived(exchange("kv", 9, stat_c))
    stat_d[0] = slots(stat_c)
    arrived(exchange("tp", 6, stat_d))
    inv = factor_of(slots(stat_d)) * 0.5
    result_ref[...] = (stream[tp] + own_cols * inv * post3_ref[pl.ds(tp, 1), :]).astype(BF16)

    for copy in sends:
        copy.wait_send()


UNROLL = 4


def one_kernel(
    n_kv,
    n_tp,
    tokens,
    gain_pre1,
    gain_post1,
    w_gate1,
    w_up1,
    w_down1,
    gain_pre2,
    gain_post2,
    w_query,
    w_key,
    w_value,
    w_forget,
    forget_bias,
    w_out,
    keys_t,
    values_t,
    decays,
    gain_pre3,
    gain_post3,
    w_gate2,
    w_up2,
    w_down2,
):
    seqs = tokens.shape[0]
    rows_dev, hidden = w_gate1.shape
    blocks = hidden // LANES
    kv_cols = w_key.shape[1]
    query_cols = w_query.shape[1]
    positions = keys_t.shape[3]
    gains = [
        g.reshape(n_tp, LANES)
        for g in (gain_pre1, gain_post1, gain_pre2, gain_post2, gain_pre3, gain_post3)
    ]
    keys = keys_t.reshape(seqs, kv_cols, positions)
    values = values_t.reshape(seqs, kv_cols, positions)
    big = [w_gate1, w_up1, w_down1, w_query, w_key, w_value, w_forget]
    big += [w_out, keys, values, w_gate2, w_up2, w_down2]
    vmem = pl.BlockSpec(memory_space=pltpu.VMEM)
    anywhere = pl.BlockSpec(memory_space=pl.ANY)
    row = (seqs, LANES)
    held = [pltpu.VMEM(w.shape, BF16) for w in big]
    held[6] = pltpu.VMEM((rows_dev, w_forget.shape[1]), BF16)
    gu_shape = (n_kv, blocks, seqs, 2 * LANES)
    scratch = held + [
        pltpu.SemaphoreType.DMA((len(big),)),
        pltpu.VMEM((n_tp,) + row, BF16),
        pltpu.VMEM((n_tp,) + row, F32),
        pltpu.VMEM(gu_shape[1:], F32),
        pltpu.VMEM(gu_shape, BF16),
        pltpu.VMEM(gu_shape, BF16),
        pltpu.VMEM((n_kv,) + row, F32),
        pltpu.VMEM((n_kv,) + row, F32),
        pltpu.VMEM((n_kv,) + row, F32),
        pltpu.VMEM((n_kv,) + row, F32),
        pltpu.VMEM((n_kv,) + row, F32),
        pltpu.VMEM((n_kv,) + row, F32),
        pltpu.VMEM((n_tp,) + row, F32),
        pltpu.VMEM((n_kv, seqs, query_cols + 2 * kv_cols), F32),
        pltpu.VMEM((2, seqs, kv_cols), F32),
        pltpu.VMEM((2, seqs, kv_cols), F32),
        pltpu.VMEM((2,) + row, F32),
        pltpu.VMEM((n_kv, 2, seqs, kv_cols + 2 * LANES), F32),
        pltpu.VMEM((seqs, 2, kv_cols + 3 * LANES), F32),
        pltpu.VMEM((6, n_tp) + row, F32),
        pltpu.VMEM((n_tp,) + row, F32),
        pltpu.VMEM((n_tp,) + row, F32),
        pltpu.VMEM((n_tp,) + row, F32),
        pltpu.VMEM((n_tp,) + row, F32),
        pltpu.VMEM((n_tp,) + row, F32),
        pltpu.SemaphoreType.DMA((10, n_kv - 1)),
        pltpu.SemaphoreType.DMA((10, n_kv - 1)),
        pltpu.SemaphoreType.DMA((7, n_tp - 1)),
        pltpu.SemaphoreType.DMA((7, n_tp - 1)),
    ]
    return pl.pallas_call(
        functools.partial(layer_kernel, n_kv, n_tp),
        out_shape=jax.ShapeDtypeStruct(row, BF16),
        in_specs=[vmem] * 7
        + [pl.BlockSpec(memory_space=pltpu.SMEM), vmem]
        + [anywhere] * len(big),
        out_specs=vmem,
        scratch_shapes=scratch,
        compiler_params=pltpu.CompilerParams(
            collective_id=0, has_side_effects=True, vmem_limit_bytes=60 * 1024 * 1024
        ),
    )(tokens, *gains, forget_bias, decays, *big)


def solution(mesh):
    placed = (
        P(None, ("kv", "tp")),
        P("kv"),
        P("kv"),
        P("kv", "tp"),
        P("kv", "tp"),
        P("tp", "kv"),
        P("kv"),
        P("kv"),
        P("kv", "tp"),
        P("kv", "tp"),
        P("kv", "tp"),
        P(),
        P("tp"),
        P("tp", "kv"),
        P(None, "tp", None, "kv"),
        P(None, "tp", None, "kv"),
        P(None, "tp", "kv"),
        P("kv"),
        P("kv"),
        P("kv", "tp"),
        P("kv", "tp"),
        P("tp", "kv"),
    )
    n_kv, n_tp = mesh.shape["kv"], mesh.shape["tp"]

    def local(*arrays):
        tokens, w_gate, w_query, w_key = arrays[0], arrays[3], arrays[8], arrays[9]
        shapes = {
            "cols": tokens.shape[1],
            "hidden": w_gate.shape[1],
            "kv_cols": w_key.shape[1],
            "kv_dev": w_key.shape[1] // HEAD,
            "rows_dev": w_gate.shape[0],
            "query_cols": w_query.shape[1],
        }
        if fits(mesh, shapes):
            return one_kernel(n_kv, n_tp, *arrays)
        return body(*arrays)

    return jax.shard_map(
        local, mesh=mesh, in_specs=placed, out_specs=P(None, ("kv", "tp")), check_vma=False
    )
```

```python
import functools

import jax
import jax.numpy as jnp
from jax import lax
from jax.experimental import pallas as pl
from jax.experimental.pallas import tpu as pltpu
from jax.sharding import PartitionSpec as P

D = 4096
HEAD = 64


EPSILON = 1e-06


def joined(x, axis, combine):
    everything = jax.tree.map(lambda part: lax.all_gather(part, axis), x)
    initial = jax.tree.map(lambda part: part[0], everything)

    def lap(k, so_far):
        return combine(so_far, jax.tree.map(lambda part: part[k], everything))

    return lax.fori_loop(1, lax.axis_size(axis), lap, initial)


def add_branch(row_block, mixed, weight_out, gain_post, factor):
    branch = lax.psum(jnp.dot(mixed, weight_out, preferred_element_type=jnp.float32), "tp")
    summed = lax.psum(jnp.sum(branch * branch, axis=1), "kv")
    inv_rms = lax.rsqrt(summed / D + EPSILON)[:, None]
    return (row_block.astype(jnp.float32) + factor * branch * inv_rms * gain_post[None, :]).astype(
        jnp.bfloat16
    )


def channel_mix(row_block, gain_pre, gain_post, w_gate, w_up, w_down, factor):
    widened = row_block.astype(jnp.float32)
    scaled = (widened * gain_pre[None, :]).astype(jnp.bfloat16)
    square = jnp.sum(widened * widened, axis=1)
    gate_part = jnp.dot(scaled, w_gate, preferred_element_type=jnp.float32)
    up_part = jnp.dot(scaled, w_up, preferred_element_type=jnp.float32)
    gate, upward, summed = lax.psum((gate_part, up_part, square), "kv")
    inv_rms = lax.rsqrt(summed / D + EPSILON)[:, None]
    hidden = (jax.nn.silu(gate * inv_rms) * (upward * inv_rms)).astype(jnp.bfloat16)
    return add_branch(row_block, hidden, w_down, gain_post, factor)


def merge_softmax(former, latter):
    joined_max = jnp.maximum(former[0], latter[0])
    former_scale = jnp.exp(former[0] - joined_max)
    latter_scale = jnp.exp(latter[0] - joined_max)
    return (
        joined_max,
        former[1] * former_scale + latter[1] * latter_scale,
        former[2] * former_scale[..., None] + latter[2] * latter_scale[..., None],
    )


def token_mix(
    row_block,
    gain_pre,
    gain_post,
    w_query,
    w_key,
    w_value,
    w_forget,
    forget_bias,
    w_out,
    keys_t,
    values_t,
    decays,
):
    widened = row_block.astype(jnp.float32)
    scaled = (widened * gain_pre[None, :]).astype(jnp.bfloat16)
    square = jnp.sum(widened * widened, axis=1)
    rows_dev = row_block.shape[1]
    seq_count = row_block.shape[0]
    kv_dev = w_key.shape[1] // HEAD
    group_size = w_query.shape[1] // w_key.shape[1]
    forget_cols = lax.dynamic_slice(
        w_forget,
        (lax.axis_index("kv") * rows_dev, lax.axis_index("tp") * kv_dev),
        (rows_dev, kv_dev),
    )
    query_part = jnp.dot(scaled, w_query, preferred_element_type=jnp.float32)
    key_part = jnp.dot(scaled, w_key, preferred_element_type=jnp.float32)
    value_part = jnp.dot(scaled, w_value, preferred_element_type=jnp.float32)
    forget_part = jnp.dot(scaled, forget_cols, preferred_element_type=jnp.float32)
    query_rows, fresh_key, value_new, forget, summed = lax.psum(
        (query_part, key_part, value_part, forget_part, square), "kv"
    )
    inv_rms = lax.rsqrt(summed / D + EPSILON)[:, None]
    query_rows = (
        (query_rows * inv_rms).astype(jnp.bfloat16).reshape(seq_count, kv_dev, group_size, HEAD)
    )
    fresh_key = (fresh_key * inv_rms).astype(jnp.bfloat16).reshape(seq_count, kv_dev, HEAD)
    value_new = (value_new * inv_rms).astype(jnp.bfloat16).reshape(seq_count, kv_dev, HEAD)
    log_gate = jax.nn.log_sigmoid(forget * inv_rms + forget_bias[None, :])
    scores = jnp.einsum(
        "bkgd,bkdp->bkgp", query_rows, keys_t, preferred_element_type=jnp.float32
    ) * HEAD ** (-0.5)
    scores = scores + decays[:, :, None, :] + log_gate[:, :, None, None]
    block_max = jnp.max(scores, axis=3)
    weights = jnp.exp(scores - block_max[..., None])
    block_sum = jnp.sum(weights, axis=3)
    block_values = jnp.einsum(
        "bkgp,bkdp->bkgd",
        weights.astype(jnp.bfloat16),
        values_t,
        preferred_element_type=jnp.float32,
    )
    block_max, block_sum, block_values = joined(
        (block_max, block_sum, block_values), "kv", merge_softmax
    )
    own_score = jnp.einsum(
        "tlvi,tli->tlv", query_rows, fresh_key, preferred_element_type=jnp.float32
    ) * HEAD ** (-0.5)
    peak_all = jnp.maximum(block_max, own_score)
    block_scale = jnp.exp(block_max - peak_all)
    own_weight = jnp.exp(own_score - peak_all)
    denominator = block_sum * block_scale + own_weight
    numerator = block_values * block_scale[..., None]
    numerator = numerator + own_weight[..., None] * value_new.astype(jnp.float32)[:, :, None, :]
    attended = (numerator / denominator[..., None]).astype(jnp.bfloat16)
    attended = attended.reshape(seq_count, kv_dev * group_size * HEAD)
    return add_branch(row_block, attended, w_out, gain_post, 1.0)


def body(
    tokens,
    gain_pre1,
    gain_post1,
    w_gate1,
    w_up1,
    w_down1,
    gain_pre2,
    gain_post2,
    w_query,
    w_key,
    w_value,
    w_forget,
    forget_bias,
    w_out,
    keys_t,
    values_t,
    decays,
    gain_pre3,
    gain_post3,
    w_gate2,
    w_up2,
    w_down2,
):
    row_block = lax.all_gather(tokens, "tp", axis=1, tiled=True)
    stream = channel_mix(row_block, gain_pre1, gain_post1, w_gate1, w_up1, w_down1, 0.5)
    stream = token_mix(
        stream,
        gain_pre2,
        gain_post2,
        w_query,
        w_key,
        w_value,
        w_forget,
        forget_bias,
        w_out,
        keys_t,
        values_t,
        decays,
    )
    stream = channel_mix(stream, gain_pre3, gain_post3, w_gate2, w_up2, w_down2, 0.5)
    own_cols = stream.shape[1] // lax.axis_size("tp")
    result = lax.dynamic_slice_in_dim(stream, lax.axis_index("tp") * own_cols, own_cols, 1)
    return result


LANES = 128
F32 = jnp.float32
BF16 = jnp.bfloat16


def fits(mesh, shapes):
    return (
        shapes["cols"] == LANES
        and shapes["hidden"] % LANES == 0
        and shapes["kv_cols"] % LANES == 0
        and shapes["kv_dev"] <= 8
        and shapes["rows_dev"] % (2 * LANES) == 0
        and shapes["query_cols"] == 2 * shapes["kv_cols"]
    )


def layer_kernel(
    n_kv,
    n_tp,
    tokens_ref,
    pre1_ref,
    post1_ref,
    pre2_ref,
    post2_ref,
    pre3_ref,
    post3_ref,
    bias_ref,
    decays_ref,
    gate1_hbm,
    up1_hbm,
    down1_hbm,
    query_hbm,
    key_hbm,
    value_hbm,
    forget_hbm,
    out_hbm,
    keys_hbm,
    values_hbm,
    gate2_hbm,
    up2_hbm,
    down2_hbm,
    result_ref,
    gate1,
    up1,
    down1,
    wq,
    wk,
    wv,
    wf,
    wo,
    keys,
    values,
    gate2,
    up2,
    down2,
    load_sems,
    token_buf,
    stream,
    own_gu,
    gu_a,
    gu_b,
    aux_a,
    aux_b,
    aux_c,
    stat_a,
    stat_b,
    stat_c,
    stat_d,
    qkv_buf,
    grouped_q,
    fresh,
    own_buf,
    soft_buf,
    per_seq,
    branch_buf,
    rs_a,
    rs_b,
    rs_c,
    ag_a,
    ag_b,
    kv_send,
    kv_recv,
    tp_send,
    tp_recv,
):
    kv = lax.axis_index("kv")
    tp = lax.axis_index("tp")
    seqs = tokens_ref.shape[0]
    rows_dev = n_tp * LANES
    kv_cols = wk.shape[1]
    kv_dev = kv_cols // HEAD
    blocks = gate1.shape[1] // LANES

    pairs = (
        (gate1_hbm, gate1),
        (up1_hbm, up1),
        (down1_hbm, down1),
        (query_hbm, wq),
        (key_hbm, wk),
        (value_hbm, wv),
        (forget_hbm.at[:, pl.ds(pl.multiple_of(kv * rows_dev, rows_dev), rows_dev)], wf),
        (keys_hbm, keys),
        (values_hbm, values),
        (out_hbm, wo),
        (gate2_hbm, gate2),
        (up2_hbm, up2),
        (down2_hbm, down2),
    )
    loads = [
        pltpu.make_async_copy(source, target, load_sems.at[i])
        for i, (source, target) in enumerate(pairs)
    ]
    for load in loads:
        load.start()

    barrier = pltpu.get_barrier_semaphore()
    for off in range(1, n_kv):
        pl.semaphore_signal(
            barrier,
            inc=1,
            device_id={"kv": lax.rem(kv + off, n_kv)},
            device_id_type=pl.DeviceIdType.MESH,
        )
    for off in range(1, n_tp):
        pl.semaphore_signal(
            barrier,
            inc=1,
            device_id={"tp": lax.rem(tp + off, n_tp)},
            device_id_type=pl.DeviceIdType.MESH,
        )
    pl.semaphore_wait(barrier, n_kv + n_tp - 2)

    sends = []

    def place(buf, slot, span):
        return buf.at[slot] if span is None else buf.at[slot, pl.ds(*span)]

    def exchange(axis, number, buf, source=None, span=None):
        me, n, ssem, rsem = (
            (kv, n_kv, kv_send, kv_recv) if axis == "kv" else (tp, n_tp, tp_send, tp_recv)
        )
        copies = []
        for off in range(1, n):
            peer = lax.rem(me + off, n)
            copy = pltpu.make_async_remote_copy(
                src_ref=place(buf, 0, span) if source is None else source(peer),
                dst_ref=place(buf, off, span),
                send_sem=ssem.at[number, off - 1],
                recv_sem=rsem.at[number, off - 1],
                device_id={axis: peer},
                device_id_type=pl.DeviceIdType.MESH,
            )
            copy.start()
            copies.append(copy)
        sends.extend(copies)
        return copies

    def arrived(copies):
        for copy in copies:
            copy.wait_recv()

    def slots(buf):
        total = buf[0].astype(F32)
        for off in range(1, buf.shape[0]):
            total += buf[off].astype(F32)
        return total

    def slot_of(place):
        return lax.rem(tp - place + n_tp, n_tp)

    def scaled_stream(gain_ref):
        scaled = [
            (stream[j] * gain_ref[j : j + 1, :]).astype(BF16) for j in range(n_tp)
        ]
        square = stream[0] * stream[0]
        for j in range(1, n_tp):
            square += stream[j] * stream[j]
        return jnp.concatenate(scaled, axis=1), jnp.sum(square, axis=1, keepdims=True)

    def factor_of(total_square):
        return lax.rsqrt(total_square * (1.0 / (n_kv * rows_dev)) + EPSILON)

    def hidden_units(gain_ref, gate_w, up_w, waits, gu_buf, aux_buf, gu_numbers, aux_number):
        scaled, square = scaled_stream(gain_ref)
        aux_buf[0] = jnp.broadcast_to(square, (seqs, LANES))
        aux_copies = exchange("kv", aux_number, aux_buf)
        for load in waits:
            load.wait()

        half = blocks - blocks // 2
        spans = ((0, half), (half, blocks - half))
        copies = []
        for number, (low, count) in zip(gu_numbers, spans):
            for j in range(low, low + count):
                cols = slice(j * LANES, (j + 1) * LANES)
                both = jnp.concatenate([gate_w[:, cols], up_w[:, cols]], axis=1)
                part = jnp.dot(scaled, both, preferred_element_type=F32)
                own_gu[j] = part
                gu_buf[0, j] = part.astype(BF16)
            copies.append(exchange("kv", number, gu_buf, span=(low, count)))
        arrived(aux_copies)
        inv = factor_of(slots(aux_buf))
        hidden = []
        for part_copies, (low, count) in zip(copies, spans):
            arrived(part_copies)
            for j in range(low, low + count):
                total = own_gu[j]
                for off in range(1, n_kv):
                    total += gu_buf[off, j].astype(F32)
                gate = total[:, :LANES] * inv
                upward = total[:, LANES:] * inv
                hidden.append((gate / (1.0 + jnp.exp(-gate)) * upward).astype(BF16))
        return jnp.concatenate(hidden, axis=1)

    def branch_sum(mixed, weight, rs_buf, number):
        for j in range(n_tp // 2):
            cols = slice(2 * j * LANES, 2 * (j + 1) * LANES)
            part = jnp.dot(mixed, weight[:, cols], preferred_element_type=F32)
            branch_buf[number, 2 * j] = part[:, :LANES]
            branch_buf[number, 2 * j + 1] = part[:, LANES:]
        copies = exchange("tp", number, rs_buf, lambda peer: branch_buf.at[number, peer])
        total = branch_buf[number, tp]
        arrived(copies)
        for off in range(1, n_tp):
            total += rs_buf[off]
        return total

    def add_branch_all(own_cols, gain_ref, factor, ag_buf, ag_number, stat_buf, stat_number):
        ag_buf[0] = own_cols
        arrived(exchange("tp", ag_number, ag_buf))
        square = ag_buf[0] * ag_buf[0]
        for off in range(1, n_tp):
            square += ag_buf[off] * ag_buf[off]
        stat_buf[0] = jnp.broadcast_to(jnp.sum(square, axis=1, keepdims=True), (seqs, LANES))
        arrived(exchange("kv", stat_number, stat_buf))
        inv = factor_of(slots(stat_buf)) * factor
        for j in range(n_tp):
            branch = ag_buf[slot_of(j)]
            stream[j] = (
                (stream[j] + branch * inv * gain_ref[j : j + 1, :]).astype(BF16).astype(F32)
            )

    arrived(exchange("tp", 0, token_buf, lambda peer: tokens_ref))
    token_buf[0] = tokens_ref[...]
    for j in range(n_tp):
        stream[j] = token_buf[slot_of(j)].astype(F32)
    hidden = hidden_units(pre1_ref, gate1, up1, loads[0:2], gu_a, aux_a, (0, 10), 1)
    loads[2].wait()
    own_cols = branch_sum(hidden, down1, rs_a, 1)
    add_branch_all(own_cols, post1_ref, 0.5, ag_a, 2, stat_a, 2)

    scaled, square = scaled_stream(pre2_ref)
    for load in loads[3:7]:
        load.wait()
    forget = lax.dot_general(
        scaled, wf[...], (((1,), (1,)), ((), ())), preferred_element_type=F32
    )
    lane = lax.broadcasted_iota(jnp.int32, (seqs, LANES), 1)
    column = lax.broadcasted_iota(jnp.int32, forget.shape, 1)
    aux = jnp.broadcast_to(square, (seqs, LANES))
    for k in range(kv_dev):
        picked = jnp.sum(
            jnp.where(column == tp * kv_dev + k, forget, 0.0), axis=1, keepdims=True
        )
        aux = jnp.where(lane == k, picked, aux)
    aux_b[0] = aux
    aux_copies = exchange("kv", 3, aux_b)
    query_cols = wq.shape[1]
    step = 2 * LANES
    for j in range(query_cols // step):
        qkv_buf[0, :, j * step : (j + 1) * step] = jnp.dot(
            scaled, wq[:, j * step : (j + 1) * step], preferred_element_type=F32
        )
    qkv_buf[0, :, query_cols : query_cols + kv_cols] = jnp.dot(
        scaled, wk[...], preferred_element_type=F32
    )
    qkv_buf[0, :, query_cols + kv_cols :] = jnp.dot(scaled, wv[...], preferred_element_type=F32)
    qkv_copies = exchange("kv", 4, qkv_buf)

    row_at = lax.broadcasted_iota(jnp.int32, (query_cols, kv_cols), 0)
    col_at = lax.broadcasted_iota(jnp.int32, (query_cols, kv_cols), 1)
    selects = [
        jnp.where(
            row_at == (lax.div(col_at, HEAD) * 2 + g) * HEAD + lax.rem(col_at, HEAD), 1.0, 0.0
        ).astype(BF16)
        for g in range(2)
    ]
    arrived(aux_copies)
    aux = slots(aux_b)
    inv = factor_of(aux[:, kv_dev : kv_dev + 1])
    bias = jnp.zeros((seqs, LANES), F32)
    for k in range(kv_dev):
        bias = jnp.where(lane == k, bias_ref[k], bias)
    logit = aux * inv + bias
    log_gate = jnp.minimum(logit, 0.0) - jnp.log(1.0 + jnp.exp(-jnp.abs(logit)))
    log_gate = jnp.where(lane < kv_dev, log_gate, 0.0)
    arrived(qkv_copies)
    qkv = (slots(qkv_buf) * inv).astype(BF16)
    queries = qkv[:, :query_cols]
    for g in range(2):
        grouped_q[g] = jnp.dot(queries, selects[g], preferred_element_type=F32)
    fresh[0] = qkv[:, query_cols : query_cols + kv_cols].astype(F32)
    fresh[1] = qkv[:, query_cols + kv_cols :].astype(F32)
    loads[7].wait()
    loads[8].wait()

    heads = 2 * kv_dev
    head_row = lax.broadcasted_iota(jnp.int32, (heads, kv_cols), 0)
    head_col = lax.div(lax.broadcasted_iota(jnp.int32, (heads, kv_cols), 1), HEAD)
    diagonal = lax.rem(head_row, kv_dev) == head_col
    first_group = head_row < kv_dev
    stat_row = lax.broadcasted_iota(jnp.int32, (heads, LANES), 0)
    stat_lane = lax.broadcasted_iota(jnp.int32, (heads, LANES), 1)
    stat_diag = lax.rem(stat_row, kv_dev) == stat_lane

    def folded(x, g):
        return jnp.sum(x[g * kv_dev : (g + 1) * kv_dev], axis=0, keepdims=True)

    def sequence(b):
        q0 = grouped_q[0, pl.ds(b, 1), :]
        q1 = grouped_q[1, pl.ds(b, 1), :]
        spread = jnp.where(diagonal, jnp.where(first_group, q0, q1), 0.0)
        scores = jnp.dot(spread.astype(BF16), keys[b], preferred_element_type=F32)
        decay = decays_ref[b]
        scores = scores * HEAD ** (-0.5) + jnp.concatenate([decay, decay], axis=0)
        block_max = jnp.max(scores, axis=1, keepdims=True)
        weights = jnp.exp(scores - block_max)
        block_sum = jnp.sum(weights, axis=1, keepdims=True)
        block_values = lax.dot_general(
            weights.astype(BF16), values[b], (((1,), (1,)), ((), ())), preferred_element_type=F32
        )
        block_values = jnp.where(diagonal, block_values, 0.0)
        own = jnp.sum(spread * fresh[0, pl.ds(b, 1), :], axis=1, keepdims=True) * HEAD ** (-0.5)
        max_at = jnp.where(stat_diag, block_max, 0.0)
        sum_at = jnp.where(stat_diag, block_sum, 0.0)
        own_at = jnp.where(stat_diag, own, 0.0)
        found = jnp.concatenate([block_values, max_at, sum_at, own_at], axis=1)
        per_seq[b] = jnp.concatenate([folded(found, 0), folded(found, 1)], axis=0)

    def sequences(i, carry):
        for u in range(UNROLL):
            sequence(i * UNROLL + u)
        return carry

    lax.fori_loop(0, seqs // UNROLL, sequences, 0)
    width = kv_cols + 2 * LANES
    for g in range(2):
        for b in range(seqs):
            soft_buf[0, g, b : b + 1, :] = per_seq[b, g : g + 1, :width]
            own_buf[g, b : b + 1, :] = per_seq[b, g : g + 1, width:]
    soft_copies = exchange("kv", 5, soft_buf)
    arrived(soft_copies)

    wide_col = lax.div(lax.broadcasted_iota(jnp.int32, (seqs, kv_cols), 1), HEAD)

    def widened(x):
        wide = jnp.broadcast_to(x[:, 0:1], (seqs, kv_cols))
        for k in range(1, kv_dev):
            wide = jnp.where(wide_col == k, x[:, k : k + 1], wide)
        return wide

    attended = None
    for g in range(2):
        maxima = [
            soft_buf[off, g, :, kv_cols : kv_cols + LANES] + log_gate for off in range(n_kv)
        ]
        peak = own_buf[g]
        for maximum in maxima:
            peak = jnp.maximum(peak, maximum)
        own_weight = jnp.exp(own_buf[g] - peak)
        denominator = own_weight
        numerator = widened(own_weight) * fresh[1]
        for off in range(n_kv):
            scale = jnp.exp(maxima[off] - peak)
            denominator += scale * soft_buf[off, g, :, kv_cols + LANES :]
            numerator += widened(scale) * soft_buf[off, g, :, :kv_cols]
        part = (numerator / widened(denominator)).astype(BF16)
        moved = lax.dot_general(
            part, selects[g], (((1,), (1,)), ((), ())), preferred_element_type=F32
        )
        attended = moved if attended is None else attended + moved
    loads[9].wait()
    own_cols = branch_sum(attended.astype(BF16), wo, rs_b, 3)
    add_branch_all(own_cols, post2_ref, 1.0, ag_b, 4, stat_b, 6)

    hidden = hidden_units(pre3_ref, gate2, up2, loads[10:12], gu_b, aux_c, (7, 11), 8)
    loads[12].wait()
    own_cols = branch_sum(hidden, down2, rs_c, 5)
    square = jnp.sum(own_cols * own_cols, axis=1, keepdims=True)
    stat_c[0] = jnp.broadcast_to(square, (seqs, LANES))
    arrived(exchange("kv", 9, stat_c))
    stat_d[0] = slots(stat_c)
    arrived(exchange("tp", 6, stat_d))
    inv = factor_of(slots(stat_d)) * 0.5
    result_ref[...] = (stream[tp] + own_cols * inv * post3_ref[pl.ds(tp, 1), :]).astype(BF16)

    for copy in sends:
        copy.wait_send()


UNROLL = 6


def one_kernel(
    n_kv,
    n_tp,
    tokens,
    gain_pre1,
    gain_post1,
    w_gate1,
    w_up1,
    w_down1,
    gain_pre2,
    gain_post2,
    w_query,
    w_key,
    w_value,
    w_forget,
    forget_bias,
    w_out,
    keys_t,
    values_t,
    decays,
    gain_pre3,
    gain_post3,
    w_gate2,
    w_up2,
    w_down2,
):
    seqs = tokens.shape[0]
    rows_dev, hidden = w_gate1.shape
    blocks = hidden // LANES
    kv_cols = w_key.shape[1]
    query_cols = w_query.shape[1]
    positions = keys_t.shape[3]
    gains = [
        g.reshape(n_tp, LANES)
        for g in (gain_pre1, gain_post1, gain_pre2, gain_post2, gain_pre3, gain_post3)
    ]
    keys = keys_t.reshape(seqs, kv_cols, positions)
    values = values_t.reshape(seqs, kv_cols, positions)
    big = [w_gate1, w_up1, w_down1, w_query, w_key, w_value, w_forget.T]
    big += [w_out, keys, values, w_gate2, w_up2, w_down2]
    vmem = pl.BlockSpec(memory_space=pltpu.VMEM)
    anywhere = pl.BlockSpec(memory_space=pl.ANY)
    row = (seqs, LANES)
    held = [pltpu.VMEM(w.shape, BF16) for w in big]
    held[6] = pltpu.VMEM((w_forget.shape[1], rows_dev), BF16)
    gu_shape = (n_kv, blocks, seqs, 2 * LANES)
    scratch = held + [
        pltpu.SemaphoreType.DMA((len(big),)),
        pltpu.VMEM((n_tp,) + row, BF16),
        pltpu.VMEM((n_tp,) + row, F32),
        pltpu.VMEM(gu_shape[1:], F32),
        pltpu.VMEM(gu_shape, BF16),
        pltpu.VMEM(gu_shape, BF16),
        pltpu.VMEM((n_kv,) + row, F32),
        pltpu.VMEM((n_kv,) + row, F32),
        pltpu.VMEM((n_kv,) + row, F32),
        pltpu.VMEM((n_kv,) + row, F32),
        pltpu.VMEM((n_kv,) + row, F32),
        pltpu.VMEM((n_kv,) + row, F32),
        pltpu.VMEM((n_tp,) + row, F32),
        pltpu.VMEM((n_kv, seqs, query_cols + 2 * kv_cols), F32),
        pltpu.VMEM((2, seqs, kv_cols), F32),
        pltpu.VMEM((2, seqs, kv_cols), F32),
        pltpu.VMEM((2,) + row, F32),
        pltpu.VMEM((n_kv, 2, seqs, kv_cols + 2 * LANES), F32),
        pltpu.VMEM((seqs, 2, kv_cols + 3 * LANES), F32),
        pltpu.VMEM((6, n_tp) + row, F32),
        pltpu.VMEM((n_tp,) + row, F32),
        pltpu.VMEM((n_tp,) + row, F32),
        pltpu.VMEM((n_tp,) + row, F32),
        pltpu.VMEM((n_tp,) + row, F32),
        pltpu.VMEM((n_tp,) + row, F32),
        pltpu.SemaphoreType.DMA((12, n_kv - 1)),
        pltpu.SemaphoreType.DMA((12, n_kv - 1)),
        pltpu.SemaphoreType.DMA((7, n_tp - 1)),
        pltpu.SemaphoreType.DMA((7, n_tp - 1)),
    ]
    return pl.pallas_call(
        functools.partial(layer_kernel, n_kv, n_tp),
        out_shape=jax.ShapeDtypeStruct(row, BF16),
        in_specs=[vmem] * 7
        + [pl.BlockSpec(memory_space=pltpu.SMEM), vmem]
        + [anywhere] * len(big),
        out_specs=vmem,
        scratch_shapes=scratch,
        compiler_params=pltpu.CompilerParams(
            collective_id=0, has_side_effects=True, vmem_limit_bytes=60 * 1024 * 1024
        ),
    )(tokens, *gains, forget_bias, decays, *big)


def solution(mesh):
    placed = (
        P(None, ("kv", "tp")),
        P("kv"),
        P("kv"),
        P("kv", "tp"),
        P("kv", "tp"),
        P("tp", "kv"),
        P("kv"),
        P("kv"),
        P("kv", "tp"),
        P("kv", "tp"),
        P("kv", "tp"),
        P(),
        P("tp"),
        P("tp", "kv"),
        P(None, "tp", None, "kv"),
        P(None, "tp", None, "kv"),
        P(None, "tp", "kv"),
        P("kv"),
        P("kv"),
        P("kv", "tp"),
        P("kv", "tp"),
        P("tp", "kv"),
    )
    n_kv, n_tp = mesh.shape["kv"], mesh.shape["tp"]

    def local(*arrays):
        tokens, w_gate, w_query, w_key = arrays[0], arrays[3], arrays[8], arrays[9]
        shapes = {
            "cols": tokens.shape[1],
            "hidden": w_gate.shape[1],
            "kv_cols": w_key.shape[1],
            "kv_dev": w_key.shape[1] // HEAD,
            "rows_dev": w_gate.shape[0],
            "query_cols": w_query.shape[1],
        }
        if fits(mesh, shapes):
            return one_kernel(n_kv, n_tp, *arrays)
        return body(*arrays)

    return jax.shard_map(
        local, mesh=mesh, in_specs=placed, out_specs=P(None, ("kv", "tp")), check_vma=False
    )
```
